768 devices in a mesh: fs: 12 (over z), rep: 8 (over y), tp: 8 (over x, core).
Axes of the slice: x: 4, y: 8, z: 12, core: 2. Of those that a mesh axis runs over, the one named last changes fastest.
Arguments:
- saved_input: bfloat16 [61440, 3072], P(('fs', 'rep')), may hold values from -20 to 20
- key_cotangent: bfloat16 [61440, 1024], P(('fs', 'rep'), 'tp'), may hold values from -0.015625 to 0.015625
- value_cotangent: bfloat16 [61440, 2048], P(('fs', 'rep'), 'tp'), may hold values from -0.015625 to 0.015625
- key_factor: bfloat16 [3072, 256], replicated, may hold values from -0.375 to 0.375
- value_factor: bfloat16 [3072, 256], replicated, may hold values from -0.375 to 0.375
- key_weight: float32 [3072, 1024], P(('fs', 'rep'), 'tp'), may hold values from -0.109375 to 0.109375
- value_weight: float32 [3072, 2048], P(('fs', 'rep'), 'tp'), may hold values from -0.109375 to 0.109375
- key_first: float32 [256, 1024], P(None, 'tp'), as said below
- key_second: float32 [256, 1024], P(None, 'tp'), may hold values from 0.05 to 1
- value_first: float32 [256, 2048], P(None, 'tp'), as said below
- value_second: float32 [256, 2048], P(None, 'tp'), may hold values from 0.05 to 1
Outputs:
- key_weight_new: float32 [3072, 1024], P(('fs', 'rep'), 'tp')
- value_weight_new: float32 [3072, 2048], P(('fs', 'rep'), 'tp')
- key_first_new: float32 [256, 1024], P(None, 'tp')
- key_second_new: float32 [256, 1024], P(None, 'tp')
- value_first_new: float32 [256, 2048], P(None, 'tp')
- value_second_new: float32 [256, 2048], P(None, 'tp')
- key_step: float32 [3072, 1024], P(('fs', 'rep'), 'tp')
- value_step: float32 [3072, 2048], P(('fs', 'rep'), 'tp')
- key_copy: bfloat16 [3072, 1024], P(None, 'tp')
- value_copy: bfloat16 [3072, 2048], P(None, 'tp')
The draws below stay inside these ranges and needn't reach their ends.
Inputs may be any that keep to these rules, and one draw needn't show every extreme that they name: `key_first`: real-valued moments whose scale differs from head to head. `value_first`: real-valued moments whose scale differs from head to head.
All inputs are finite; a program needn't handle non-finite values.
Results may differ from the reference program's by a relative error of at most 0.004.
Values may be sent and summed in bfloat16 or wider, within the bound.
A program may use at most 64 MiB of HBM per device.

```python
import math
import jax
import jax.numpy as jnp
from jax import lax

D = 3072
HEADS = 8
HK = 128
HV = 256
DK = 1024
DV = 2048
RK = 256
RV = 256
TOKENS = 61440


def head_scaled(key, row_count, head_count, head_width):
    scale_key, value_key = jax.random.split(key)
    spread = jnp.exp(jax.random.uniform(scale_key, (head_count,), jnp.float32, -1.4, 1.4))
    entries = jax.random.normal(value_key, (row_count, head_count, head_width), jnp.float32)
    return (entries * spread[None, :, None]).reshape(row_count, head_count * head_width)


def draw_key_first(key, part):
    return head_scaled(jax.random.fold_in(key, 3), RK, HEADS, HK)


def draw_value_first(key, part):
    return head_scaled(jax.random.fold_in(key, 7), RV, HEADS, HV)


def spiked(values, key, source, target, shards_of, factor):
    owner, partner = [(jnp.arange(values.shape[position]) // (values.shape[position] // shards_of)).reshape([-1 if axis == position else 1 for axis in range(values.ndim)]) for position in (source, target)]
    chosen = jax.random.permutation(key, shards_of)[partner]
    strong = (owner == chosen) | (owner == (partner + shards_of // 2) % shards_of)
    return jnp.where(strong, factor * values, values)


def steps_of(stream_key, extent, shards, smallest, largest):
    factor_of, own = 1.0, jax.random.fold_in(stream_key, 6)
    for axis_at, blocks in shards:
        draws = jnp.exp(jax.random.uniform(jax.random.fold_in(own, axis_at), (blocks,), jnp.float32, smallest / len(shards), largest / len(shards)))
        factor_of = factor_of * jnp.repeat(draws, extent[axis_at] // blocks).reshape([-1 if axis == axis_at else 1 for axis in range(len(extent))])
    return factor_of


def centred(rng, dims, deviation, limit, cuts=(), dtype=jnp.bfloat16):
    loudness = steps_of(rng, dims, cuts, -0.22, 0.18) if cuts else 1.0
    values = jax.random.normal(rng, dims, jnp.float32) * deviation * loudness
    return jnp.minimum(jnp.maximum(values, -limit), limit).astype(dtype)


def heavy_noise(own_key, shape, width, most, cuts, heavy, held_as=jnp.bfloat16):
    values = width * jax.random.normal(own_key, shape, jnp.float32)
    if cuts:
        values = values * steps_of(own_key, shape, cuts, -0.22, 0.18)
    return jnp.clip(spiked(values, jax.random.fold_in(own_key, 3), *heavy), -most, most).astype(held_as)


def setup_inputs(seed: int = 0) -> dict:
    streams_of = jax.random.split(jax.random.key(seed), 12)
    saved_input = heavy_noise(streams_of[0], (TOKENS, D), 1.0, 20.0, ((0, 96),), (0, 1, 96, 4.75))
    key_cotangent = centred(streams_of[1], (TOKENS, DK), ((D * TOKENS // RK) ** -0.5), 0.015625, ((0, 96), (1, 8)))
    value_cotangent = centred(streams_of[2], (TOKENS, DV), ((D * TOKENS // RV) ** -0.5), 0.015625, ((0, 96), (1, 8)))
    key_factor = centred(streams_of[3], (D, RK), RK ** -0.5, 0.375)
    value_factor = centred(streams_of[4], (D, RV), RV ** -0.5, 0.375)
    key_weight = centred(streams_of[5], (D, DK), D ** -0.5, 0.109375, ((0, 96), (1, 8)), jnp.float32)
    value_weight = centred(streams_of[6], (D, DV), D ** -0.5, 0.109375, ((0, 96), (1, 8)), jnp.float32)
    key_first = draw_key_first(jax.random.fold_in(streams_of[11], 71), 0)
    key_second = jnp.clip(jnp.exp(math.log(1.0) - 2.9957323 * jax.random.uniform(streams_of[8], (RK, DK), jnp.float32) ** steps_of(streams_of[8], (RK, DK), ((1, 8),), -0.2, 0.2)), 0.05, 1.0)
    value_first = draw_value_first(jax.random.fold_in(streams_of[11], 71), 0)
    value_second = jnp.clip(jnp.exp(math.log(1.0) - 2.9957323 * jax.random.uniform(streams_of[10], (RV, DV), jnp.float32) ** steps_of(streams_of[10], (RV, DV), ((1, 8),), -0.2, 0.2)), 0.05, 1.0)
    return dict(saved_input=saved_input, key_cotangent=key_cotangent, value_cotangent=value_cotangent, key_factor=key_factor, value_factor=value_factor, key_weight=key_weight, value_weight=value_weight, key_first=key_first, key_second=key_second, value_first=value_first, value_second=value_second)


first_decay = 0.8
second_decay = 0.9
epsilon = 1e-08
learn_rate = 0.01

def projected(saved_input, cotangent, factor):
    basis = jnp.dot(saved_input, factor, preferred_element_type=jnp.float32)
    return lax.dot_general(basis, cotangent.astype(jnp.float32), (((0,), (0,)), ((), ())), precision=lax.Precision.HIGHEST)

def moments(projection, first, second):
    first_new = first_decay * first + (1.0 - first_decay) * projection
    second_new = second_decay * second + (1.0 - second_decay) * projection * projection
    normed = first_new / (jnp.sqrt(second_new) + epsilon)
    return (first_new, second_new, normed)

def reference(saved_input, key_cotangent, value_cotangent, key_factor, value_factor, key_weight, value_weight, key_first, key_second, value_first, value_second):
    key_projected = projected(saved_input, key_cotangent, key_factor)
    value_projected = projected(saved_input, value_cotangent, value_factor)
    key_first_new, key_second_new, key_normed = moments(key_projected, key_first, key_second)
    value_first_new, value_second_new, value_normed = moments(value_projected, value_first, value_second)
    squares = jnp.sum(key_normed * key_normed) + jnp.sum(value_normed * value_normed)
    entries = jnp.float32(RK * DK + RV * DV)
    shrink = jnp.sqrt(entries / (entries + squares))
    key_step = shrink * jnp.dot(key_factor.astype(jnp.float32), key_normed, precision=lax.Precision.HIGHEST)
    value_step = shrink * jnp.dot(value_factor.astype(jnp.float32), value_normed, precision=lax.Precision.HIGHEST)
    key_weight_new = key_weight - learn_rate * key_step
    value_weight_new = value_weight - learn_rate * value_step
    return (key_weight_new, value_weight_new, key_first_new, key_second_new, value_first_new, value_second_new, key_step, value_step, key_weight_new.astype(jnp.bfloat16), value_weight_new.astype(jnp.bfloat16))
```

```python
import jax
import jax.numpy as jnp
from jax import lax
from jax.experimental import pallas as pl
from jax.experimental.pallas import tpu as pltpu
from jax.sharding import PartitionSpec as P

MESH = pl.DeviceIdType.MESH
D, DK, DV, RK, RV = 3072, 1024, 2048, 256, 256
NZ, NY, NT = 12, 8, 8
TOK = 640
KC, VC = 128, 256
NC = KC + VC
ROWS = 32
KCHUNKS = 4
KSIZE = D // KCHUNKS

first_decay = 0.8
second_decay = 0.9
epsilon = 1e-08
learn_rate = 0.01


def kernel(
    x_hbm, ck_hbm, cv_hbm, fk_hbm, fv_hbm, wk_hbm, wv_hbm, m1k_hbm, m2k_hbm, m1v_hbm, m2v_hbm,
    wkn_hbm, wvn_hbm, m1kn_hbm, m2kn_hbm, m1vn_hbm, m2vn_hbm, sk_hbm, sv_hbm, kcopy_hbm, vcopy_hbm,
    xs, cs_k, cs_v, fk, fv, wk, wv, m1, m2, basis, part, rs1_send, rs1_recv, rs2_send, rs2_recv,
    ag, kg, vg, normed, acc, kout, vout, sq, sq_recv, ok, ov, osk, osv,
    in_sem, out_sem, r1s, r1r, r2s, r2r, a1s, a1r, a2s, a2r, k1s, k1r, v1s, v1r, krs, krr, vrs, vrr, ts, tr,
):
    z, y, t = lax.axis_index("fs"), lax.axis_index("rep"), lax.axis_index("tp")

    def zpeer(d):
        return (lax.rem(z + d, NZ), y, t)

    def ypeer(d):
        return (z, lax.rem(y + d, NY), t)

    def tpeer(d):
        return (z, y, lax.rem(t + d, NT))

    sends = []

    def send(src, dst, ssem, rsem, peer):
        copy = pltpu.make_async_remote_copy(
            src_ref=src, dst_ref=dst, send_sem=ssem, recv_sem=rsem, device_id=peer, device_id_type=MESH
        )
        copy.start()
        sends.append(copy)
        return copy

    def arrived(ref, ssem, rsem, peer):
        pltpu.make_async_remote_copy(
            src_ref=ref, dst_ref=ref, send_sem=ssem, recv_sem=rsem, device_id=peer, device_id_type=MESH
        ).wait_recv()

    loads = {}

    def load(name, src, dst):
        copy = pltpu.make_async_copy(src, dst, in_sem.at[len(loads)])
        copy.start()
        loads[name] = copy

    load("wk", wk_hbm, wk)
    load("wv", wv_hbm, wv)
    for c in range(KCHUNKS):
        ks = pl.ds(c * KSIZE, KSIZE)
        load(f"fk{c}", fk_hbm.at[ks], fk.at[ks])
        load(f"fv{c}", fv_hbm.at[ks], fv.at[ks])
        load(f"x{c}", x_hbm.at[:, ks], xs.at[:, ks])
    load("ck", ck_hbm, cs_k)
    load("cv", cv_hbm, cs_v)
    load("m1k", m1k_hbm, m1.at[0])
    load("m2k", m2k_hbm, m2.at[0])
    for c in range(2):
        cols = pl.ds(c * 128, 128)
        load(f"m1v{c}", m1v_hbm.at[:, cols], m1.at[1 + c])
        load(f"m2v{c}", m2v_hbm.at[:, cols], m2.at[1 + c])

    barrier = pltpu.get_barrier_semaphore()
    for d in range(1, NZ):
        pl.semaphore_signal(barrier, inc=1, device_id=zpeer(d), device_id_type=MESH)
    for d in range(1, NY):
        pl.semaphore_signal(barrier, inc=1, device_id=ypeer(d), device_id_type=MESH)
    for d in range(1, NT):
        pl.semaphore_signal(barrier, inc=1, device_id=tpeer(d), device_id_type=MESH)

    loads["wk"].wait()
    loads["wv"].wait()
    kg[z, y] = wk[...].astype(jnp.bfloat16)
    vg[z, y] = wv[...].astype(jnp.bfloat16)

    def basis_chunk(c):
        ks = slice(c * KSIZE, (c + 1) * KSIZE)
        for name in ("fk", "fv", "x"):
            loads[f"{name}{c}"].wait()
        xc = xs[:, ks]
        for f, cols in ((fk, slice(0, RK)), (fv, slice(RK, RK + RV))):
            term = jnp.dot(xc, f[ks, :], preferred_element_type=jnp.float32)
            if c == 0:
                basis[:, cols] = term
            else:
                basis[:, cols] += term

    basis_chunk(0)
    basis_chunk(1)

    pl.semaphore_wait(barrier, NZ - 1 + NY - 1 + NT - 1)
    for d in range(1, NY):
        send(vg.at[z, y], vg.at[z, y], v1s.at[d - 1], v1r.at[d - 1], ypeer(d))
    for d in range(1, NZ):
        send(kg.at[z, y], kg.at[z, y], k1s.at[d - 1], k1r.at[d - 1], zpeer(d))

    basis_chunk(2)
    basis_chunk(3)

    loads["ck"].wait()
    loads["cv"].wait()
    dims = (((0,), (0,)), ((), ()))
    for cols, cot, outs in (
        (slice(0, RK), cs_k, slice(0, KC)),
        (slice(RK, RK + RV), cs_v, slice(KC, NC)),
    ):
        b = basis[:, cols]
        upper = b.astype(jnp.bfloat16)
        lower = (b - upper.astype(jnp.float32)).astype(jnp.bfloat16)
        p = lax.dot_general(upper, cot[...], dims, preferred_element_type=jnp.float32)
        p += lax.dot_general(lower, cot[...], dims, preferred_element_type=jnp.float32)
        part[:, :, outs] = p.reshape(NY, ROWS, outs.stop - outs.start)
        rs1_send[:, :, outs] = p.reshape(NY, ROWS, outs.stop - outs.start).astype(jnp.bfloat16)

    for d in range(1, NY):
        peer = ypeer(d)
        send(rs1_send.at[peer[1]], rs1_recv.at[d - 1], r1s.at[d - 1], r1r.at[d - 1], peer)

    def half(c, n):
        return pl.ds(c * n, n)

    def kblock(owner, c):
        return kg.at[half(c, NZ // 2), owner]

    def vblock(owner, c):
        return vg.at[owner, half(c, NY // 2)]

    def ring(block, me, n, peer_of, ssem, rsem):
        steps = n // 2

        def owner_of(direction, hops):
            return lax.rem(me + (n - hops if direction == 0 else hops), n)

        def carries(direction, s, c):
            return s < steps or c == direction

        def put(direction, s, c):
            ref = block(owner_of(direction, s - 1), c)
            send(ref, ref, ssem.at[direction, s - 1, c], rsem.at[direction, s - 1, c],
                 peer_of(1 if direction == 0 else n - 1))

        def take(direction, s, c):
            ref = block(owner_of(direction, s), c)
            arrived(ref, ssem.at[direction, s - 1, c], rsem.at[direction, s - 1, c],
                    peer_of(1 if direction == 0 else n - 1))

        ticks = []
        for s in range(1, steps + 1):
            for c in range(2):
                for direction in range(2):
                    if not carries(direction, s, c):
                        continue

                    def tick(direction=direction, s=s, c=c):
                        take(direction, s, c)
                        if s < steps and carries(direction, s + 1, c):
                            put(direction, s + 1, c)

                    ticks.append(tick)

        def start():
            for c in range(2):
                for direction in range(2):
                    if carries(direction, 1, c):
                        put(direction, 1, c)

        return start, ticks

    vstart, vticks = ring(vblock, z, NZ, zpeer, vrs, vrr)
    kstart, kticks = ring(kblock, y, NY, ypeer, krs, krr)

    def run(ticks, count):
        for _ in range(min(count, len(ticks))):
            ticks.pop(0)()

    for d in range(1, NY):
        arrived(vg.at[z, lax.rem(y + NY - d, NY)], v1s.at[d - 1], v1r.at[d - 1], ypeer(d))
    vstart()
    for d in range(1, NZ):
        arrived(kg.at[lax.rem(z + NZ - d, NZ), y], k1s.at[d - 1], k1r.at[d - 1], zpeer(d))
    kstart()

    total = part[y]
    for d in range(1, NY):
        arrived(rs1_recv.at[d - 1], r1s.at[d - 1], r1r.at[d - 1], ypeer(d))
        total += rs1_recv[d - 1].astype(jnp.float32)
    for i in range(NZ):
        rs2_send[i] = total[8 * (i // 3) : 8 * (i // 3) + 8, 128 * (i % 3) : 128 * (i % 3) + 128]
    for d in range(1, NZ):
        peer = zpeer(d)
        send(rs2_send.at[peer[0]], rs2_recv.at[d - 1], r2s.at[d - 1], r2r.at[d - 1], peer)

    run(vticks, 4)
    run(kticks, 4)

    tile = rs2_send[z]
    for d in range(1, NZ):
        arrived(rs2_recv.at[d - 1], r2s.at[d - 1], r2r.at[d - 1], zpeer(d))
        tile += rs2_recv[d - 1]
    ag[y, z] = tile
    for d in range(1, NZ):
        send(ag.at[y, z], ag.at[y, z], a1s.at[d - 1], a1r.at[d - 1], zpeer(d))

    run(vticks, 4)
    run(kticks, 4)

    for d in range(1, NZ):
        arrived(ag.at[y, lax.rem(z + NZ - d, NZ)], a1s.at[d - 1], a1r.at[d - 1], zpeer(d))
    for d in range(1, NY):
        send(ag.at[y], ag.at[y], a2s.at[d - 1], a2r.at[d - 1], ypeer(d))

    run(vticks, 4)
    run(kticks, 4)
    run(vticks, 4)

    for d in range(1, NY):
        arrived(ag.at[lax.rem(y + NY - d, NY)], a2s.at[d - 1], a2r.at[d - 1], ypeer(d))

    outs = []

    def store(src, dst):
        copy = pltpu.make_async_copy(src, dst, out_sem.at[len(outs)])
        copy.start()
        outs.append(copy)

    squares = jnp.zeros((8, 128), jnp.float32)
    for g in range(3):
        for name in (("m1k", "m2k"), ("m1v0", "m2v0"), ("m1v1", "m2v1"))[g]:
            loads[name].wait()
        proj = jnp.concatenate([ag[b, 3 * i + g] for b in range(NY) for i in range(4)], axis=0)
        first_new = first_decay * m1[g] + (1.0 - first_decay) * proj
        second_new = second_decay * m2[g] + (1.0 - second_decay) * proj * proj
        m1[g] = first_new
        m2[g] = second_new
        n = first_new / (jnp.sqrt(second_new) + epsilon)
        squares += jnp.sum((n * n).reshape(RK // 8, 8, 128), axis=0)
        upper = n.astype(jnp.bfloat16)
        lower = (n - upper.astype(jnp.float32)).astype(jnp.bfloat16)
        normed[:, 128 * g : 128 * g + 128] = upper
        normed[:, NC + 128 * g : NC + 128 * g + 128] = lower
    sq[...] = squares
    for d in range(1, NT):
        send(sq, sq_recv.at[d - 1], ts.at[d - 1], tr.at[d - 1], tpeer(d))
    store(m1.at[0], m1kn_hbm)
    store(m2.at[0], m2kn_hbm)
    for c in range(2):
        cols = pl.ds(c * 128, 128)
        store(m1.at[1 + c], m1vn_hbm.at[:, cols])
        store(m2.at[1 + c], m2vn_hbm.at[:, cols])

    def rows_of(b):
        return pl.ds(pl.multiple_of(b * 256, 256), 256)

    @pl.loop(0, NZ)
    def _(b):
        rows = rows_of(b)
        wide = jnp.dot(
            fk[rows, :],
            jnp.concatenate([normed[:, 0:KC], normed[:, NC : NC + KC]], axis=1),
            preferred_element_type=jnp.float32,
        )
        acc[rows, 0:KC] = wide[:, :KC] + wide[:, KC:]
        acc[rows, KC:NC] = jnp.dot(
            fv[rows, :], normed[:, KC:NC], preferred_element_type=jnp.float32
        ) + jnp.dot(fv[rows, :], normed[:, NC + KC :], preferred_element_type=jnp.float32)

    run(vticks, 100)
    run(kticks, 100)

    squares = sq[...]
    for d in range(1, NT):
        arrived(sq_recv.at[d - 1], ts.at[d - 1], tr.at[d - 1], tpeer(d))
        squares += sq_recv[d - 1]
    whole = jnp.sum(jnp.sum(squares, axis=0, keepdims=True), axis=1, keepdims=True)
    entries = float(RK * DK + RV * DV)
    shrink = jnp.sqrt(entries / (entries + whole))

    mine = pl.ds(pl.multiple_of((z * NY + y) * ROWS, ROWS), ROWS)
    step_k = shrink * acc[mine, 0:KC]
    step_v = shrink * acc[mine, KC:NC]
    osk[...] = step_k
    osv[...] = step_v
    ok[...] = wk[...] - learn_rate * step_k
    ov[...] = wv[...] - learn_rate * step_v
    store(osk, sk_hbm)
    store(osv, sv_hbm)
    store(ok, wkn_hbm)
    store(ov, wvn_hbm)

    for b in range(NZ):
        rows = slice(b * 256, b * 256 + 256)
        kw = kg[b].reshape(256, KC).astype(jnp.float32)
        kout[rows, :] = (kw - learn_rate * (shrink * acc[rows, 0:KC])).astype(jnp.bfloat16)
        vw = vg[b].reshape(256, VC).astype(jnp.float32)
        vout[rows, :] = (vw - learn_rate * (shrink * acc[rows, KC:NC])).astype(jnp.bfloat16)
        store(kout.at[pl.ds(b * 256, 256)], kcopy_hbm.at[pl.ds(b * 256, 256)])
        store(vout.at[pl.ds(b * 256, 256)], vcopy_hbm.at[pl.ds(b * 256, 256)])

    for copy in sends:
        copy.wait_send()
    for copy in outs:
        copy.wait()


def body(*args):
    f32, bf16 = jnp.float32, jnp.bfloat16
    V, S = pltpu.VMEM, pltpu.SemaphoreType.DMA
    outs = [
        ((ROWS, KC), f32), ((ROWS, VC), f32), ((RK, KC), f32), ((RK, KC), f32), ((RV, VC), f32), ((RV, VC), f32),
        ((ROWS, KC), f32), ((ROWS, VC), f32), ((D, KC), bf16), ((D, VC), bf16),
    ]
    return pl.pallas_call(
        kernel,
        name="projected_update",
        out_shape=[jax.ShapeDtypeStruct(s, dt) for s, dt in outs],
        in_specs=[pl.BlockSpec(memory_space=pl.ANY)] * 11,
        out_specs=[pl.BlockSpec(memory_space=pl.ANY)] * 10,
        scratch_shapes=[
            V((TOK, D), bf16), V((TOK, KC), bf16), V((TOK, VC), bf16), V((D, RK), bf16), V((D, RV), bf16),
            V((ROWS, KC), f32), V((ROWS, VC), f32), V((3, RK, 128), f32), V((3, RK, 128), f32),
            V((TOK, RK + RV), f32), V((NY, ROWS, NC), f32), V((NY, ROWS, NC), bf16), V((NY - 1, ROWS, NC), bf16),
            V((NZ, 8, 128), f32), V((NZ - 1, 8, 128), f32), V((NY, NZ, 8, 128), f32),
            V((NZ, NY, ROWS, KC), bf16), V((NZ, NY, ROWS, VC), bf16), V((RK, 2 * NC), bf16), V((D, NC), f32),
            V((D, KC), bf16), V((D, VC), bf16), V((8, 128), f32), V((NT - 1, 8, 128), f32),
            V((ROWS, KC), f32), V((ROWS, VC), f32), V((ROWS, KC), f32), V((ROWS, VC), f32),
            S((2 + 3 * KCHUNKS + 2 + 6,)), S((6 + 4 + 2 * NZ,)),
            S((NY - 1,)), S((NY - 1,)), S((NZ - 1,)), S((NZ - 1,)), S((NZ - 1,)), S((NZ - 1,)), S((NY - 1,)), S((NY - 1,)),
            S((NZ - 1,)), S((NZ - 1,)), S((NY - 1,)), S((NY - 1,)),
            S((2, NY // 2, 2)), S((2, NY // 2, 2)), S((2, NZ // 2, 2)), S((2, NZ // 2, 2)),
            S((NT - 1,)), S((NT - 1,)),
        ],
        compiler_params=pltpu.CompilerParams(collective_id=0, has_side_effects=True),
    )(*args)


def solution(mesh):
    tokens, rows, cols = P(("fs", "rep"), None), P(("fs", "rep"), "tp"), P(None, "tp")
    in_specs = (tokens, rows, rows, P(), P(), rows, rows, cols, cols, cols, cols)
    out_specs = (rows, rows, cols, cols, cols, cols, rows, rows, cols, cols)
    return jax.shard_map(body, mesh=mesh, in_specs=in_specs, out_specs=out_specs, check_vma=False)
```

```python
import jax
import jax.numpy as jnp
from jax import lax
from jax.experimental import pallas as pl
from jax.experimental.pallas import tpu as pltpu
from jax.sharding import PartitionSpec as P

MESH = pl.DeviceIdType.MESH
D, DK, DV, RK, RV = 3072, 1024, 2048, 256, 256
NZ, NY, NT = 12, 8, 8
TOK = 640
KC, VC = 128, 256
NC = KC + VC
ROWS = 32
KCHUNKS = 4
KSIZE = D // KCHUNKS
STEP = 768
KCH, VCH = 2, 4
HELD = 2 * D * NC + 4 * D * RK + 4 * ROWS * NC + 8 * RK * NC + 4 * RK * NC + 4096
VMEM_MAIN = 67043328 - HELD - 72 * 1024

first_decay = 0.8
second_decay = 0.9
epsilon = 1e-08
learn_rate = 0.01


def kernel(
    x_hbm, ck_hbm, cv_hbm, fk_hbm, fv_hbm, wk_hbm, wv_hbm, m1k_hbm, m2k_hbm, m1v_hbm, m2v_hbm,
    kg, vg, fk, fv, wk, wv, m1, m2, normed, shrink_out,
    xs, cs_k, cs_v, basis, part, rs1_send, rs1_recv, rs2_send, rs2_recv, ag, qt, qy,
    in_sem, r1s, r1r, r2s, r2r, a1s, a1r, a2s, a2r, k1s, k1r, v1s, v1r, krs, krr, vrs, vrr, ts, tr, us, ur,
):
    z, y, t = lax.axis_index("fs"), lax.axis_index("rep"), lax.axis_index("tp")

    def zpeer(d):
        return (lax.rem(z + d, NZ), y, t)

    def ypeer(d):
        return (z, lax.rem(y + d, NY), t)

    def tpeer(d):
        return (z, y, lax.rem(t + d, NT))

    sends = []

    def send(src, dst, ssem, rsem, peer):
        copy = pltpu.make_async_remote_copy(
            src_ref=src, dst_ref=dst, send_sem=ssem, recv_sem=rsem, device_id=peer, device_id_type=MESH
        )
        copy.start()
        sends.append(copy)
        return copy

    def arrived(ref, ssem, rsem, peer):
        pltpu.make_async_remote_copy(
            src_ref=ref, dst_ref=ref, send_sem=ssem, recv_sem=rsem, device_id=peer, device_id_type=MESH
        ).wait_recv()

    loads = {}

    def load(name, src, dst):
        copy = pltpu.make_async_copy(src, dst, in_sem.at[len(loads)])
        copy.start()
        loads[name] = copy

    load("wk", wk_hbm, wk)
    load("wv", wv_hbm, wv)
    for c in range(KCHUNKS):
        ks = pl.ds(c * KSIZE, KSIZE)
        load(f"fk{c}", fk_hbm.at[ks], fk.at[ks])
        load(f"fv{c}", fv_hbm.at[ks], fv.at[ks])
        load(f"x{c}", x_hbm.at[:, ks], xs.at[:, ks])
    load("ck", ck_hbm, cs_k)
    load("cv", cv_hbm, cs_v)
    load("m1k", m1k_hbm, m1.at[0])
    load("m2k", m2k_hbm, m2.at[0])
    for c in range(2):
        cols = pl.ds(c * 128, 128)
        load(f"m1v{c}", m1v_hbm.at[:, cols], m1.at[1 + c])
        load(f"m2v{c}", m2v_hbm.at[:, cols], m2.at[1 + c])

    barrier = pltpu.get_barrier_semaphore()
    for d in range(1, NZ):
        pl.semaphore_signal(barrier, inc=1, device_id=zpeer(d), device_id_type=MESH)
    for d in range(1, NY):
        pl.semaphore_signal(barrier, inc=1, device_id=ypeer(d), device_id_type=MESH)
    for d in range(1, NT):
        pl.semaphore_signal(barrier, inc=1, device_id=tpeer(d), device_id_type=MESH)

    loads["wk"].wait()
    loads["wv"].wait()
    kg[z, y] = wk[...].astype(jnp.bfloat16)
    vg[z, y] = wv[...].astype(jnp.bfloat16)

    def basis_chunk(c):
        ks = slice(c * KSIZE, (c + 1) * KSIZE)
        for name in ("fk", "fv", "x"):
            loads[f"{name}{c}"].wait()
        xc = xs[:, ks]
        for f, cols in ((fk, slice(0, RK)), (fv, slice(RK, RK + RV))):
            term = jnp.dot(xc, f[ks, :], preferred_element_type=jnp.float32)
            if c == 0:
                basis[:, cols] = term
            else:
                basis[:, cols] += term

    basis_chunk(0)
    pl.semaphore_wait(barrier, NZ - 1 + NY - 1 + NT - 1)
    for d in range(1, NY):
        send(vg.at[z, y], vg.at[z, y], v1s.at[d - 1], v1r.at[d - 1], ypeer(d))
    for d in range(1, NZ):
        send(kg.at[z, y], kg.at[z, y], k1s.at[d - 1], k1r.at[d - 1], zpeer(d))
    for c in range(1, KCHUNKS):
        basis_chunk(c)

    loads["ck"].wait()
    loads["cv"].wait()
    dims = (((0,), (0,)), ((), ()))
    for cols, cot, outs in (
        (slice(0, RK), cs_k, slice(0, KC)),
        (slice(RK, RK + RV), cs_v, slice(KC, NC)),
    ):
        b = basis[:, cols]
        upper = b.astype(jnp.bfloat16)
        lower = (b - upper.astype(jnp.float32)).astype(jnp.bfloat16)
        p = lax.dot_general(upper, cot[...], dims, preferred_element_type=jnp.float32)
        p += lax.dot_general(lower, cot[...], dims, preferred_element_type=jnp.float32)
        part[:, :, outs] = p.reshape(NY, ROWS, outs.stop - outs.start)
        rs1_send[:, :, outs] = p.reshape(NY, ROWS, outs.stop - outs.start).astype(jnp.bfloat16)

    for d in range(1, NY):
        peer = ypeer(d)
        send(rs1_send.at[peer[1]], rs1_recv.at[d - 1], r1s.at[d - 1], r1r.at[d - 1], peer)

    def ring(block, chunks, me, n, peer_of, ssem, rsem):
        steps = n // 2

        def owner_of(direction, hops):
            return lax.rem(me + (n - hops if direction == 0 else hops), n)

        def carries(direction, s, c):
            return s < steps or (c < chunks // 2) == (direction == 0)

        def put(direction, s, c):
            ref = block(owner_of(direction, s - 1), c)
            at = direction, s - 1, c
            send(ref, ref, ssem.at[at], rsem.at[at], peer_of(1 if direction == 0 else n - 1))

        def take(direction, s, c):
            ref = block(owner_of(direction, s), c)
            at = direction, s - 1, c
            arrived(ref, ssem.at[at], rsem.at[at], peer_of(1 if direction == 0 else n - 1))
            if s < steps and carries(direction, s + 1, c):
                put(direction, s + 1, c)

        def round_(s, chosen=range(chunks)):
            for c in chosen:
                for direction in range(2):
                    if s == 0:
                        put(direction, 1, c)
                    elif carries(direction, s, c):
                        take(direction, s, c)

        return round_

    kround = ring(lambda o, c: kg.at[pl.ds(c * (NZ // KCH), NZ // KCH), o], KCH, y, NY, ypeer, krs, krr)
    vround = ring(lambda o, c: vg.at[o, pl.ds(c * (NY // VCH), NY // VCH)], VCH, z, NZ, zpeer, vrs, vrr)

    for d in range(1, NY):
        arrived(vg.at[z, lax.rem(y + NY - d, NY)], v1s.at[d - 1], v1r.at[d - 1], ypeer(d))
    vround(0)

    total = part[y]
    for d in range(1, NY):
        arrived(rs1_recv.at[d - 1], r1s.at[d - 1], r1r.at[d - 1], ypeer(d))
        total += rs1_recv[d - 1].astype(jnp.float32)
    for i in range(NZ):
        rs2_send[i] = total[8 * (i // 3) : 8 * (i // 3) + 8, 128 * (i % 3) : 128 * (i % 3) + 128]
    for d in range(1, NZ):
        peer = zpeer(d)
        send(rs2_send.at[peer[0]], rs2_recv.at[d - 1], r2s.at[d - 1], r2r.at[d - 1], peer)

    for d in range(1, NZ):
        arrived(kg.at[lax.rem(z + NZ - d, NZ), y], k1s.at[d - 1], k1r.at[d - 1], zpeer(d))
    kround(0)
    vround(1)
    kround(1)
    vround(2)

    tile = rs2_send[z]
    for d in range(1, NZ):
        arrived(rs2_recv.at[d - 1], r2s.at[d - 1], r2r.at[d - 1], zpeer(d))
        tile += rs2_recv[d - 1]
    ag[y, z] = tile
    for d in range(1, NZ):
        send(ag.at[y, z], ag.at[y, z], a1s.at[d - 1], a1r.at[d - 1], zpeer(d))

    kround(2)
    vround(3)
    kround(3)
    vround(4)

    for d in range(1, NZ):
        arrived(ag.at[y, lax.rem(z + NZ - d, NZ)], a1s.at[d - 1], a1r.at[d - 1], zpeer(d))
    halves = pl.ds(0, NZ // 2), pl.ds(NZ // 2, NZ // 2)

    def far(hops):
        return lax.rem(y + NY + hops, NY)

    def ag_send(slot, ref, hops):
        send(ref, ref, a2s.at[slot], a2r.at[slot], ypeer(NY + hops))

    def ag_arrived(slot, ref):
        arrived(ref, a2s.at[slot], a2r.at[slot], ypeer(1))

    for slot, hops in ((2, 2), (3, -2), (0, 1), (1, -1)):
        ag_send(slot, ag.at[y], hops)

    def normed_of(proj, first, second):
        first_new = first_decay * first + (1.0 - first_decay) * proj
        second_new = second_decay * second + (1.0 - second_decay) * proj * proj
        return first_new, second_new, first_new / (jnp.sqrt(second_new) + epsilon)

    for name in ("m1k", "m2k", "m1v0", "m2v0", "m1v1", "m2v1"):
        loads[name].wait()
    squares = jnp.zeros((8, 128), jnp.float32)
    for i in range(NZ):
        at = pl.ds(pl.multiple_of(ROWS * y + 8 * (i // 3), 8), 8)
        n = normed_of(ag[y, i], m1[i % 3, at], m2[i % 3, at])[2]
        squares += n * n
    qt[t] = squares
    for d in range(1, NT):
        send(qt.at[t], qt.at[t], ts.at[d - 1], tr.at[d - 1], tpeer(d))

    kround(4)
    vround(5)

    for slot, hops in ((2, 1), (3, -1)):
        owner = far(-2 * hops)
        ag_arrived(slot, ag.at[owner])
        ag_send(slot + 2, ag.at[owner], hops)
        half = ag.at[owner, halves[slot - 2]]
        ag_send(slot + 4, half, 2 * hops)

    for d in range(1, NT):
        arrived(qt.at[lax.rem(t + NT - d, NT)], ts.at[d - 1], tr.at[d - 1], tpeer(d))
    squares = qt[0]
    for i in range(1, NT):
        squares += qt[i]
    qy[y] = squares
    for d in range(1, NY):
        send(qy.at[y], qy.at[y], us.at[d - 1], ur.at[d - 1], ypeer(d))

    vround(6)

    for slot, hops in ((0, -1), (1, 1), (4, -3), (5, 3)):
        ag_arrived(slot, ag.at[far(hops)])
    ag_arrived(6, ag.at[far(4), halves[0]])
    ag_arrived(7, ag.at[far(4), halves[1]])

    for g in range(3):
        proj = jnp.concatenate([ag[b, 3 * i + g] for b in range(NY) for i in range(4)], axis=0)
        first_new, second_new, n = normed_of(proj, m1[g], m2[g])
        m1[g] = first_new
        m2[g] = second_new
        upper = n.astype(jnp.bfloat16)
        lower = (n - upper.astype(jnp.float32)).astype(jnp.bfloat16)
        at = (0, 256, 384)[g]
        normed[:, at : at + 128] = upper
        at = (128, 512, 640)[g]
        normed[:, at : at + 128] = lower

    for d in range(1, NY):
        arrived(qy.at[lax.rem(y + NY - d, NY)], us.at[d - 1], ur.at[d - 1], ypeer(d))
    squares = qy[0]
    for i in range(1, NY):
        squares += qy[i]
    whole = jnp.sum(jnp.sum(squares, axis=0, keepdims=True), axis=1, keepdims=True)
    entries = float(RK * DK + RV * DV)
    shrink_out[...] = jnp.broadcast_to(jnp.sqrt(entries / (entries + whole)), (8, 128))

    for copy in sends:
        copy.wait_send()


def finish(
    kg, vg, fk, fv, wk, wv, m1, m2, normed, shrink_in,
    wkn_hbm, wvn_hbm, m1kn_hbm, m2kn_hbm, m1vn_hbm, m2vn_hbm, sk_hbm, sv_hbm, kcopy_hbm, vcopy_hbm,
    kout, vout, ok, ov, osk, osv, out_sem,
):
    z, y = lax.axis_index("fs"), lax.axis_index("rep")
    outs = []

    def store(src, dst):
        copy = pltpu.make_async_copy(src, dst, out_sem.at[len(outs)])
        copy.start()
        outs.append(copy)

    store(m1.at[0], m1kn_hbm)
    store(m2.at[0], m2kn_hbm)
    for c in range(2):
        cols = pl.ds(c * 128, 128)
        store(m1.at[1 + c], m1vn_hbm.at[:, cols])
        store(m2.at[1 + c], m2vn_hbm.at[:, cols])

    shrink = shrink_in[0:1, 0:1]

    def steps_of(rows):
        wide = jnp.dot(fk[rows, :], normed[:, 0:256], preferred_element_type=jnp.float32)
        tall = jnp.dot(fv[rows, :], normed[:, 256:512], preferred_element_type=jnp.float32)
        tall += jnp.dot(fv[rows, :], normed[:, 512:768], preferred_element_type=jnp.float32)
        return shrink * (wide[:, :KC] + wide[:, KC:]), shrink * tall

    blocks = STEP // 256
    for b in range(D // STEP):
        rows = slice(b * STEP, b * STEP + STEP)
        key_step, value_step = steps_of(rows)
        kw = kg[blocks * b : blocks * b + blocks].reshape(STEP, KC).astype(jnp.float32)
        kout[rows, :] = (kw - learn_rate * key_step).astype(jnp.bfloat16)
        vw = vg[blocks * b : blocks * b + blocks].reshape(STEP, VC).astype(jnp.float32)
        vout[rows, :] = (vw - learn_rate * value_step).astype(jnp.bfloat16)
        store(kout.at[pl.ds(b * STEP, STEP)], kcopy_hbm.at[pl.ds(b * STEP, STEP)])
        store(vout.at[pl.ds(b * STEP, STEP)], vcopy_hbm.at[pl.ds(b * STEP, STEP)])

    key_step, value_step = steps_of(pl.ds(pl.multiple_of((z * NY + y) * ROWS, ROWS), ROWS))
    osk[...] = key_step
    osv[...] = value_step
    ok[...] = wk[...] - learn_rate * key_step
    ov[...] = wv[...] - learn_rate * value_step
    store(osk, sk_hbm)
    store(osv, sv_hbm)
    store(ok, wkn_hbm)
    store(ov, wvn_hbm)
    for copy in outs:
        copy.wait()


def body(*args):
    f32, bf16 = jnp.float32, jnp.bfloat16
    V, S = pltpu.VMEM, pltpu.SemaphoreType.DMA
    outs = [
        ((ROWS, KC), f32), ((ROWS, VC), f32), ((RK, KC), f32), ((RK, KC), f32), ((RV, VC), f32), ((RV, VC), f32),
        ((ROWS, KC), f32), ((ROWS, VC), f32), ((D, KC), bf16), ((D, VC), bf16),
    ]
    held = [
        V((NZ, NY, ROWS, KC), bf16), V((NZ, NY, ROWS, VC), bf16), V((D, RK), bf16), V((D, RV), bf16),
        V((ROWS, KC), f32), V((ROWS, VC), f32), V((3, RK, 128), f32), V((3, RK, 128), f32), V((RK, 2 * NC), bf16),
        V((8, 128), f32),
    ]
    held_specs = [pl.BlockSpec(memory_space=V)] * len(held)
    middle = pl.pallas_call(
        kernel,
        name="projected_update",
        out_shape=held,
        in_specs=[pl.BlockSpec(memory_space=pltpu.HBM)] * 11,
        out_specs=held_specs,
        scratch_shapes=[
            V((TOK, D), bf16), V((TOK, KC), bf16), V((TOK, VC), bf16),
            V((TOK, RK + RV), f32), V((NY, ROWS, NC), f32), V((NY, ROWS, NC), bf16), V((NY - 1, ROWS, NC), bf16),
            V((NZ, 8, 128), f32), V((NZ - 1, 8, 128), f32), V((NY, NZ, 8, 128), f32),
            V((NT, 8, 128), f32), V((NY, 8, 128), f32),
            S((2 + 3 * KCHUNKS + 2 + 6,)),
            S((NY - 1,)), S((NY - 1,)), S((NZ - 1,)), S((NZ - 1,)), S((NZ - 1,)), S((NZ - 1,)), S((8,)), S((8,)),
            S((NZ - 1,)), S((NZ - 1,)), S((NY - 1,)), S((NY - 1,)),
            S((2, NY // 2, KCH)), S((2, NY // 2, KCH)), S((2, NZ // 2, VCH)), S((2, NZ // 2, VCH)),
            S((NT - 1,)), S((NT - 1,)), S((NY - 1,)), S((NY - 1,)),
        ],
        compiler_params=pltpu.CompilerParams(collective_id=0, has_side_effects=True, vmem_limit_bytes=VMEM_MAIN),
    )(*args)
    return pl.pallas_call(
        finish,
        name="finish",
        out_shape=[jax.ShapeDtypeStruct(s, dt) for s, dt in outs],
        in_specs=held_specs,
        out_specs=[pl.BlockSpec(memory_space=pltpu.HBM)] * len(outs),
        scratch_shapes=[
            V((D, KC), bf16), V((D, VC), bf16),
            V((ROWS, KC), f32), V((ROWS, VC), f32), V((ROWS, KC), f32), V((ROWS, VC), f32),
            S((10 + 2 * (D // STEP),)),
        ],
        compiler_params=pltpu.CompilerParams(vmem_limit_bytes=16 << 20),
    )(*middle)


def solution(mesh):
    tokens, rows, cols = P(("fs", "rep"), None), P(("fs", "rep"), "tp"), P(None, "tp")
    in_specs = (tokens, rows, rows, P(), P(), rows, rows, cols, cols, cols, cols)
    out_specs = (rows, rows, cols, cols, cols, cols, rows, rows, cols, cols)
    return jax.shard_map(body, mesh=mesh, in_specs=in_specs, out_specs=out_specs, check_vma=False)
```

```python
import jax
import jax.numpy as jnp
from jax import lax
from jax.experimental import pallas as pl
from jax.experimental.pallas import tpu as pltpu
from jax.sharding import PartitionSpec as P

MESH = pl.DeviceIdType.MESH
D, DK, DV, RK, RV = 3072, 1024, 2048, 256, 256
NZ, NY, NT = 12, 8, 8
TOK = 640
KC, VC = 128, 256
NC = KC + VC
ROWS = 32
KAT = (0, 512, 1536, 2560, 3072)
KCHUNKS = len(KAT) - 1
FAR_Y = (4, 3, 5, 2, 6, 1, 7)
NEAR_FIRST_Y = (1, 7, 6, 2, 5, 3, 4)
FAR_Z = (6, 5, 7, 4, 8, 3, 9, 2, 10, 1, 11)
VALUE, VALUE_FAR, KEY, RS_REP, RS_REP_FAR, RS_FS, AG_FS, AG_FS_FAR, AG_REP, SQ_REP, SQ_TP, KEY_RING, VALUE_RING = range(13)
GROUPS = 13
NEAR, NEAR_Y = 2, 1
STEP = 512
KCH, VCH = 2, 4
HELD = 2 * D * NC + 4 * D * RK + 4 * ROWS * NC + 8 * RK * NC + 4 * RK * NC + 4096
VMEM_MAIN = 67043328 - HELD - 72 * 1024

first_decay = 0.8
second_decay = 0.9
epsilon = 1e-08
learn_rate = 0.01


def kernel(
    x_hbm, ck_hbm, cv_hbm, fk_hbm, fv_hbm, wk_hbm, wv_hbm, m1k_hbm, m2k_hbm, m1v_hbm, m2v_hbm,
    kg, vg, fk, fv, wk, wv, mm, normed, shrink_out,
    xs, cs_k, cs_v, basis, part, rs1_send, rs1_recv, rs2_send, rs2_recv, ag, qt, qy,
    in_sem, out_sems, in_sems, a2r, krr, vrr,
):
    z, y, t = lax.axis_index("fs"), lax.axis_index("rep"), lax.axis_index("tp")

    def zpeer(d):
        return (lax.rem(z + d, NZ), y, t)

    def ypeer(d):
        return (z, lax.rem(y + d, NY), t)

    def tpeer(d):
        return (z, y, lax.rem(t + d, NT))

    def copy_of(src, dst, ssem, rsem, peer):
        return pltpu.make_async_remote_copy(
            src_ref=src, dst_ref=dst, send_sem=ssem, recv_sem=rsem, device_id=peer, device_id_type=MESH
        )

    def send(src, dst, group, peer, rsem=None):
        copy_of(src, dst, out_sems.at[group], in_sems.at[group] if rsem is None else rsem, peer).start()

    def arrived(ref, group=None, rsem=None):
        copy_of(ref, ref, out_sems.at[0], in_sems.at[group] if rsem is None else rsem, zpeer(1)).wait_recv()

    def sent(ref, group):
        copy_of(ref, ref, out_sems.at[group], in_sems.at[group], zpeer(1)).wait_send()

    loads = {}

    def load(name, src, dst):
        copy = pltpu.make_async_copy(src, dst, in_sem.at[len(loads)])
        copy.start()
        loads[name] = copy

    def load_chunk(c):
        ks = pl.ds(KAT[c], KAT[c + 1] - KAT[c])
        load(f"fk{c}", fk_hbm.at[ks], fk.at[ks])
        load(f"fv{c}", fv_hbm.at[ks], fv.at[ks])
        load(f"x{c}", x_hbm.at[:, ks], xs.at[:, ks])

    load_chunk(0)
    load("wk", wk_hbm, wk)
    load("wv", wv_hbm, wv)
    for c in range(1, KCHUNKS):
        load_chunk(c)
    load("ck", ck_hbm, cs_k)
    load("cv", cv_hbm, cs_v)
    moments_sem = in_sem.at[len(loads)]
    for src, dst in (
        (m1k_hbm, 0), (m1v_hbm.at[:, pl.ds(0, 128)], 1), (m1v_hbm.at[:, pl.ds(128, 128)], 2),
        (m2k_hbm, 3), (m2v_hbm.at[:, pl.ds(0, 128)], 4), (m2v_hbm.at[:, pl.ds(128, 128)], 5),
    ):
        pltpu.make_async_copy(src, mm.at[dst], moments_sem).start()

    barrier = pltpu.get_barrier_semaphore()
    for d in range(1, NZ):
        pl.semaphore_signal(barrier, inc=1, device_id=zpeer(d), device_id_type=MESH)
    for d in range(1, NY):
        pl.semaphore_signal(barrier, inc=1, device_id=ypeer(d), device_id_type=MESH)
    for d in range(1, NT):
        pl.semaphore_signal(barrier, inc=1, device_id=tpeer(d), device_id_type=MESH)

    def basis_chunk(c):
        ks = slice(KAT[c], KAT[c + 1])
        for name in ("fk", "fv", "x"):
            loads[f"{name}{c}"].wait()
        xc = xs[:, ks]
        for f, cols in ((fk, slice(0, RK)), (fv, slice(RK, RK + RV))):
            term = jnp.dot(xc, f[ks, :], preferred_element_type=jnp.float32)
            if c == 0:
                basis[:, cols] = term
            else:
                basis[:, cols] += term

    basis_chunk(0)
    loads["wk"].wait()
    loads["wv"].wait()
    kg[z, y] = wk[...].astype(jnp.bfloat16)
    vg[z, NEAR_Y] = wv[...].astype(jnp.bfloat16)
    pl.semaphore_wait(barrier, NZ - 1 + NY - 1 + NT - 1)
    for d in NEAR_FIRST_Y:
        slot = (NEAR_Y - d) % NY
        send(vg.at[z, NEAR_Y], vg.at[z, slot], VALUE if slot < NY // 2 else VALUE_FAR, ypeer(d))
    for d in FAR_Z:
        send(kg.at[z, y], kg.at[z, y], KEY, zpeer(d))
    for c in range(1, KCHUNKS):
        basis_chunk(c)

    slots = [lax.rem(i - z + NZ + NEAR, NZ) for i in range(NZ)]
    near, beyond = pl.ds(0, NZ // 2), pl.ds(NZ // 2, NZ // 2)

    loads["ck"].wait()
    loads["cv"].wait()
    dims = (((0,), (0,)), ((), ()))
    for cols, cot, outs in (
        (slice(0, RK), cs_k, slice(0, KC)),
        (slice(RK, RK + RV), cs_v, slice(KC, NC)),
    ):
        b = basis[:, cols]
        upper = b.astype(jnp.bfloat16)
        lower = (b - upper.astype(jnp.float32)).astype(jnp.bfloat16)
        p = lax.dot_general(upper, cot[...], dims, preferred_element_type=jnp.float32)
        p += lax.dot_general(lower, cot[...], dims, preferred_element_type=jnp.float32)
        for b in range(NY):
            for i in range(outs.start // 128, NZ):
                if outs.start <= 128 * (i % 3) < outs.stop:
                    at = ROWS * b + 8 * (i // 3)
                    lanes = 128 * (i % 3) - outs.start
                    piece = p[at : at + 8, lanes : lanes + 128]
                    part[b, slots[i]] = piece
                    rs1_send[b, slots[i]] = piece.astype(jnp.bfloat16)

    for tiles, group in ((beyond, RS_REP_FAR), (near, RS_REP)):
        for d in FAR_Y:
            peer = ypeer(d)
            send(rs1_send.at[peer[1], tiles], rs1_recv.at[d - 1, tiles], group, peer)

    def ring(block, chunks, me, n, peer_of, group, rsem):
        steps = n // 2

        def owner_of(direction, hops):
            return lax.rem(me + (n - hops if direction == 0 else hops), n)

        def carries(direction, s, c):
            return s < steps or (c < chunks // 2) == (direction == 0)

        def put(direction, s, c):
            ref = block(owner_of(direction, s - 1), c)
            send(ref, ref, group, peer_of(1 if direction == 0 else n - 1), rsem.at[direction, s - 1, c])

        def take(direction, s, c):
            arrived(block(owner_of(direction, s), c), rsem=rsem.at[direction, s - 1, c])
            if s < steps and carries(direction, s + 1, c):
                put(direction, s + 1, c)

        def round_(s, chosen=range(chunks)):
            for c in chosen:
                for direction in range(2):
                    if s == 0:
                        put(direction, 1, c)
                    elif carries(direction, s, c):
                        take(direction, s, c)

        return round_

    kround = ring(lambda o, c: kg.at[pl.ds(c * (NZ // KCH), NZ // KCH), o], KCH, y, NY, ypeer, KEY_RING, krr)
    vround = ring(lambda o, c: vg.at[o, pl.ds(c * (NY // VCH), NY // VCH)], VCH, z, NZ, zpeer, VALUE_RING, vrr)

    lower, upper = range(VCH // 2), range(VCH // 2, VCH)

    arrived(vg.at[z, pl.ds(0, NY // 2 - 1)], VALUE)
    vround(0, lower)
    arrived(vg.at[z, pl.ds(NY // 2, NY // 2)], VALUE_FAR)
    vround(0, upper)
    vround(1, lower)

    for tiles, group, order in (
        (beyond, RS_REP_FAR, (6, 5, 7, 4, 8, 9)), (near, RS_REP, (3, 2, 10, 1, 11, 0)),
    ):
        arrived(rs1_recv.at[:, tiles], group)
        for d in order:
            slot = (d + NEAR) % NZ
            total = part[y, slot]
            for i in range(NY - 1):
                total += rs1_recv[i, slot].astype(jnp.float32)
            rs2_send[slot] = total
        for d in order:
            if d:
                send(rs2_send.at[(d + NEAR) % NZ], rs2_recv.at[d - 1], RS_FS, zpeer(d))

    arrived(kg.at[pl.ds(0, NZ - 1), y], KEY)
    kround(0)
    vround(1, upper)
    vround(2, lower)
    kround(1)
    vround(2, upper)
    vround(3, lower)

    tile = rs2_send[NEAR]
    arrived(rs2_recv, RS_FS)
    for d in range(1, NZ):
        tile += rs2_recv[d - 1]
    ag[y, NEAR] = tile
    for d in FAR_Z:
        slot = (NEAR - d) % NZ
        send(ag.at[y, NEAR], ag.at[y, slot], AG_FS if slot < NZ // 2 else AG_FS_FAR, zpeer(d))

    kround(2)
    vround(3, upper)
    vround(4, lower)
    kround(3)

    def ag_send(ref, hops, rsem=None):
        send(ref, ref, AG_REP, ypeer(NY + hops), rsem)

    def ag_own(p, tiles):
        for hops, which in ((2, 0), (-2, 1)):
            ag_send(ag.at[y, tiles], hops, a2r.at[which, p])
        for hops in (1, -1):
            ag_send(ag.at[y, tiles], hops)

    def ag_pass(p, tiles):
        for hops, which in ((1, 0), (-1, 1)):
            ref = ag.at[lax.rem(y + NY - 2 * hops, NY), tiles]
            arrived(ref, rsem=a2r.at[which, p])
            ag_send(ref, hops)
            if which == p:
                ag_send(ref, 2 * hops)

    arrived(ag.at[y, pl.ds(0, NZ // 2 - 1)], AG_FS)
    ag_own(0, near)

    vround(4, upper)

    arrived(ag.at[y, beyond], AG_FS_FAR)

    def normed_of(proj, first, second):
        first_new = first_decay * first + (1.0 - first_decay) * proj
        second_new = second_decay * second + (1.0 - second_decay) * proj * proj
        return first_new, second_new, first_new / (jnp.sqrt(second_new) + epsilon)

    pltpu.make_async_copy(mm, mm, moments_sem).wait()
    squares = jnp.zeros((8, 128), jnp.float32)
    for i in range(NZ):
        at = pl.ds(pl.multiple_of(ROWS * y + 8 * (i // 3), 8), 8)
        n = normed_of(ag[y, slots[i]], mm[i % 3, at], mm[3 + i % 3, at])[2]
        squares += n * n
    qy[y] = squares
    for d in FAR_Y:
        send(qy.at[y], qy.at[y], SQ_REP, ypeer(d))
    ag_own(1, beyond)

    vround(5, lower)

    ag_pass(0, near)

    vround(5, upper)

    arrived(qy.at[pl.ds(0, NY - 1)], SQ_REP)
    squares = qy[0]
    for i in range(1, NY):
        squares += qy[i]
    qt[t] = squares
    for d in range(1, NT):
        send(qt.at[t], qt.at[t], SQ_TP, tpeer(d))

    ag_pass(1, beyond)

    kround(4)
    vround(6)

    arrived(ag.at[pl.ds(0, NY - 3)], AG_REP)

    for g in range(3):
        proj = jnp.concatenate([ag[b, slots[3 * i + g]] for b in range(NY) for i in range(4)], axis=0)
        first_new, second_new, n = normed_of(proj, mm[g], mm[3 + g])
        mm[g] = first_new
        mm[3 + g] = second_new
        upper = n.astype(jnp.bfloat16)
        lower = (n - upper.astype(jnp.float32)).astype(jnp.bfloat16)
        normed[:, 128 * g : 128 * g + 128] = upper
        normed[:, NC + 128 * g : NC + 128 * g + 128] = lower

    arrived(qt.at[pl.ds(0, NT - 1)], SQ_TP)
    squares = qt[0]
    for i in range(1, NT):
        squares += qt[i]
    whole = jnp.sum(jnp.sum(squares, axis=0, keepdims=True), axis=1, keepdims=True)
    entries = float(RK * DK + RV * DV)
    shrink_out[...] = jnp.broadcast_to(jnp.sqrt(entries / (entries + whole)), (8, 128))

    sent(vg.at[z, pl.ds(0, NY // 2 - 1)], VALUE)
    sent(vg.at[z, pl.ds(NY // 2, NY // 2)], VALUE_FAR)
    sent(kg.at[pl.ds(0, NZ - 1), y], KEY)
    sent(rs1_recv.at[:, near], RS_REP)
    sent(rs1_recv.at[:, beyond], RS_REP_FAR)
    sent(rs2_recv, RS_FS)
    sent(ag.at[y, pl.ds(0, NZ // 2 - 1)], AG_FS)
    sent(ag.at[y, beyond], AG_FS_FAR)
    sent(ag.at[pl.ds(0, NY - 1)], AG_REP)
    sent(qy.at[pl.ds(0, NY - 1)], SQ_REP)
    sent(qt.at[pl.ds(0, NT - 1)], SQ_TP)
    sent(kg.at[:, pl.ds(0, NY - 1)], KEY_RING)
    sent(vg.at[pl.ds(0, NZ - 1)], VALUE_RING)


def finish(
    kg, vg, fk, fv, wk, wv, mm, normed, shrink_in,
    wkn_hbm, wvn_hbm, m1kn_hbm, m2kn_hbm, m1vn_hbm, m2vn_hbm, sk_hbm, sv_hbm, kcopy_hbm, vcopy_hbm,
    kout, vout, ok, ov, osk, osv, out_sem,
):
    z, y = lax.axis_index("fs"), lax.axis_index("rep")
    outs = []

    def store(src, dst):
        copy = pltpu.make_async_copy(src, dst, out_sem.at[len(outs)])
        copy.start()
        outs.append(copy)

    for src, dst in (
        (0, m1kn_hbm), (1, m1vn_hbm.at[:, pl.ds(0, 128)]), (2, m1vn_hbm.at[:, pl.ds(128, 128)]),
        (3, m2kn_hbm), (4, m2vn_hbm.at[:, pl.ds(0, 128)]), (5, m2vn_hbm.at[:, pl.ds(128, 128)]),
    ):
        store(mm.at[src], dst)

    shrink = shrink_in[0:1, 0:1]

    def steps_of(rows, parts):
        key_step = value_step = 0.0
        for at in parts:
            key_step += jnp.dot(fk[rows, :], normed[:, at : at + KC], preferred_element_type=jnp.float32)
            value_step += jnp.dot(fv[rows, :], normed[:, at + KC : at + NC], preferred_element_type=jnp.float32)
        return shrink * key_step, shrink * value_step

    blocks = STEP // 256
    for b in range(D // STEP):
        rows = slice(b * STEP, b * STEP + STEP)
        key_step, value_step = steps_of(rows, (0,))
        kw = kg[blocks * b : blocks * b + blocks].reshape(STEP, KC).astype(jnp.float32)
        kout[rows, :] = (kw - learn_rate * key_step).astype(jnp.bfloat16)
        vw = jnp.concatenate(
            [vg[blocks * b + i, lax.rem(j - y + NY + NEAR_Y, NY)] for i in range(blocks) for j in range(NY)], axis=0
        ).astype(jnp.float32)
        vout[rows, :] = (vw - learn_rate * value_step).astype(jnp.bfloat16)
        store(kout.at[pl.ds(b * STEP, STEP)], kcopy_hbm.at[pl.ds(b * STEP, STEP)])
        store(vout.at[pl.ds(b * STEP, STEP)], vcopy_hbm.at[pl.ds(b * STEP, STEP)])

    key_step, value_step = steps_of(pl.ds(pl.multiple_of((z * NY + y) * ROWS, ROWS), ROWS), (0, NC))
    osk[...] = key_step
    osv[...] = value_step
    ok[...] = wk[...] - learn_rate * key_step
    ov[...] = wv[...] - learn_rate * value_step
    store(osk, sk_hbm)
    store(osv, sv_hbm)
    store(ok, wkn_hbm)
    store(ov, wvn_hbm)
    for copy in outs:
        copy.wait()


def body(*args):
    f32, bf16 = jnp.float32, jnp.bfloat16
    V, S = pltpu.VMEM, pltpu.SemaphoreType.DMA
    outs = [
        ((ROWS, KC), f32), ((ROWS, VC), f32), ((RK, KC), f32), ((RK, KC), f32), ((RV, VC), f32), ((RV, VC), f32),
        ((ROWS, KC), f32), ((ROWS, VC), f32), ((D, KC), bf16), ((D, VC), bf16),
    ]
    held = [
        V((NZ, NY, ROWS, KC), bf16), V((NZ, NY, ROWS, VC), bf16), V((D, RK), bf16), V((D, RV), bf16),
        V((ROWS, KC), f32), V((ROWS, VC), f32), V((6, RK, 128), f32), V((RK, 2 * NC), bf16), V((8, 128), f32),
    ]
    held_specs = [pl.BlockSpec(memory_space=V)] * len(held)
    middle = pl.pallas_call(
        kernel,
        name="projected_update",
        out_shape=held,
        in_specs=[pl.BlockSpec(memory_space=pltpu.HBM)] * 11,
        out_specs=held_specs,
        scratch_shapes=[
            V((TOK, D), bf16), V((TOK, KC), bf16), V((TOK, VC), bf16),
            V((TOK, RK + RV), f32), V((NY, NZ, 8, 128), f32), V((NY, NZ, 8, 128), bf16), V((NY - 1, NZ, 8, 128), bf16),
            V((NZ, 8, 128), f32), V((NZ - 1, 8, 128), f32), V((NY, NZ, 8, 128), f32),
            V((NT, 8, 128), f32), V((NY, 8, 128), f32),
            S((2 + 3 * KCHUNKS + 2 + 1,)), S((GROUPS,)), S((GROUPS,)), S((2, 2)),
            S((2, NY // 2, KCH)), S((2, NZ // 2, VCH)),
        ],
        compiler_params=pltpu.CompilerParams(collective_id=0, has_side_effects=True, vmem_limit_bytes=VMEM_MAIN),
    )(*args)
    return pl.pallas_call(
        finish,
        name="finish",
        out_shape=[jax.ShapeDtypeStruct(s, dt) for s, dt in outs],
        in_specs=held_specs,
        out_specs=[pl.BlockSpec(memory_space=pltpu.HBM)] * len(outs),
        scratch_shapes=[
            V((D, KC), bf16), V((D, VC), bf16),
            V((ROWS, KC), f32), V((ROWS, VC), f32), V((ROWS, KC), f32), V((ROWS, VC), f32),
            S((10 + 2 * (D // STEP),)),
        ],
        compiler_params=pltpu.CompilerParams(vmem_limit_bytes=16 << 20),
    )(*middle)


def solution(mesh):
    tokens, rows, cols = P(("fs", "rep"), None), P(("fs", "rep"), "tp"), P(None, "tp")
    in_specs = (tokens, rows, rows, P(), P(), rows, rows, cols, cols, cols, cols)
    out_specs = (rows, rows, cols, cols, cols, cols, rows, rows, cols, cols)
    return jax.shard_map(body, mesh=mesh, in_specs=in_specs, out_specs=out_specs, check_vma=False)
```

```python
import jax
import jax.numpy as jnp
from jax import lax
from jax.experimental import pallas as pl
from jax.experimental.pallas import tpu as pltpu
from jax.sharding import PartitionSpec as P

MESH = pl.DeviceIdType.MESH
D, DK, DV, RK, RV = 3072, 1024, 2048, 256, 256
NZ, NY, NT, NX = 12, 8, 8, 4
TOK = 640
KC, VC = 128, 256
NC = KC + VC
ROWS = 32
KAT = (0, 512, 1536, 2560, 3072)
KCHUNKS = len(KAT) - 1
FAR_Y = (4, 3, 5, 2, 6, 1, 7)
NEAR_FIRST_Y = (1, 7, 6, 2, 5, 3, 4)
FAR_Z = (6, 5, 7, 4, 8, 3, 9, 2, 10, 1, 11)
VALUE, VALUE_FAR, KEY, VALUE_TWIN, KEY_TWIN, MOMENTS_TWIN, AG_TWIN, SQ_TWIN = range(8)
RS_REP, RS_REP_FAR = 8, 10
RS_FS, AG_FS, AG_FS_FAR, AG_REP, SQ_REP, SQ_TP, KEY_RING, VALUE_RING = range(12, 20)
VALUE_HOME, KEY_HOME, VALUE_RING_HOME, KEY_RING_HOME = range(20, 24)
GROUPS = 24
NEAR, NEAR_Y = 2, 1
STEP = 512
KCH, VCH = 2, 4
HELD = 4 * D * NC + 4 * D * RK + 4 * ROWS * NC + 8 * RK * NC + 4 * RK * NC + 4096
VMEM_MAIN = 67043328 - HELD - 72 * 1024

first_decay = 0.8
second_decay = 0.9
epsilon = 1e-08
learn_rate = 0.01


def kernel(
    x_hbm, ck_hbm, cv_hbm, fk_hbm, fv_hbm, wk_hbm, wv_hbm, m1k_hbm, m2k_hbm, m1v_hbm, m2v_hbm,
    kg, vg, fk, fv, wk, wv, mm, normed, shrink_out,
    xs, cs_k, cs_v, basis, part, rs1_send, rs1_recv, rs2_send, rs2_recv, ag, qt, qy, total_sq, twin_mm,
    in_sem, out_sems, in_sems, a2r, krr, vrr,
):
    z, y, t = lax.axis_index("fs"), lax.axis_index("rep"), lax.axis_index("tp")

    core = lax.rem(t, 2)
    first, second = t - core, t - core + 1
    mover, adder = core == 0, core == 1
    other = (z, y, t + 1 - 2 * core)
    x = t // 2

    def zpeer(d, tp):
        return (lax.rem(z + d, NZ), y, tp)

    def ypeer(d, tp):
        return (z, lax.rem(y + d, NY), tp)

    def copy_of(src, dst, ssem, rsem, peer):
        return pltpu.make_async_remote_copy(
            src_ref=src, dst_ref=dst, send_sem=ssem, recv_sem=rsem, device_id=peer, device_id_type=MESH
        )

    def send(src, dst, group, peer, rsem=None):
        copy_of(src, dst, out_sems.at[group], in_sems.at[group] if rsem is None else rsem, peer).start()

    def arrived(ref, group=None, rsem=None):
        copy_of(ref, ref, out_sems.at[0], in_sems.at[group] if rsem is None else rsem, other).wait_recv()

    def sent(ref, group):
        copy_of(ref, ref, out_sems.at[group], in_sems.at[group], other).wait_send()

    loads = {}

    def load(name, src, dst):
        copy = pltpu.make_async_copy(src, dst, in_sem.at[len(loads)])
        copy.start()
        loads[name] = copy

    def load_chunk(c):
        ks = pl.ds(KAT[c], KAT[c + 1] - KAT[c])
        load(f"fk{c}", fk_hbm.at[ks], fk.at[ks])
        load(f"fv{c}", fv_hbm.at[ks], fv.at[ks])
        load(f"x{c}", x_hbm.at[:, ks], xs.at[:, ks])

    load_chunk(0)
    load("wk", wk_hbm, wk)
    load("wv", wv_hbm, wv)
    for c in range(1, KCHUNKS):
        load_chunk(c)
    load("ck", ck_hbm, cs_k)
    load("cv", cv_hbm, cs_v)
    moments_sem = in_sem.at[len(loads)]
    for src, dst in (
        (m1k_hbm, 0), (m1v_hbm.at[:, pl.ds(0, 128)], 1), (m1v_hbm.at[:, pl.ds(128, 128)], 2),
        (m2k_hbm, 3), (m2v_hbm.at[:, pl.ds(0, 128)], 4), (m2v_hbm.at[:, pl.ds(128, 128)], 5),
    ):
        pltpu.make_async_copy(src, mm.at[dst], moments_sem).start()

    barrier = pltpu.get_barrier_semaphore()

    def greet(peer):
        pl.semaphore_signal(barrier, inc=1, device_id=peer, device_id_type=MESH)

    for tp in (first, second):
        for d in range(1, NZ):
            greet(zpeer(d, tp))
        for d in range(1, NY):
            greet(ypeer(d, tp))
    greet(other)

    @pl.when(adder)
    def _():
        for d in range(1, NX):
            greet((z, y, lax.rem(t + 2 * d, NT)))

    def basis_chunk(c):
        ks = slice(KAT[c], KAT[c + 1])
        for name in ("fk", "fv", "x"):
            loads[f"{name}{c}"].wait()
        xc = xs[:, ks]
        for f, cols in ((fk, slice(0, RK)), (fv, slice(RK, RK + RV))):
            term = jnp.dot(xc, f[ks, :], preferred_element_type=jnp.float32)
            if c == 0:
                basis[:, cols] = term
            else:
                basis[:, cols] += term

    basis_chunk(0)
    loads["wk"].wait()
    loads["wv"].wait()
    kg[core, NEAR, y] = wk[...].astype(jnp.bfloat16)
    vg[core, z, NEAR_Y] = wv[...].astype(jnp.bfloat16)

    @pl.when(mover)
    def _():
        pl.semaphore_wait(barrier, 2 * (NZ - 1 + NY - 1) + 1)

    @pl.when(adder)
    def _():
        pl.semaphore_wait(barrier, 2 * (NZ - 1 + NY - 1) + 1 + NX - 1)
        send(vg.at[1, z, NEAR_Y], vg.at[1, z, NEAR_Y], VALUE_TWIN, other)
        send(kg.at[1, NEAR, y], kg.at[1, NEAR, y], KEY_TWIN, other)

    for d in NEAR_FIRST_Y:
        slot = (NEAR_Y - d) % NY
        send(
            vg.at[core, z, NEAR_Y], vg.at[core, z, slot], VALUE if slot < NY // 2 else VALUE_FAR, ypeer(d, first)
        )
    for d in FAR_Z:
        send(kg.at[core, NEAR, y], kg.at[core, (NEAR - d) % NZ, y], KEY, zpeer(d, first))
    for c in range(1, KCHUNKS):
        basis_chunk(c)

    slots = [lax.rem(i - z + NZ + NEAR, NZ) for i in range(NZ)]
    near, beyond = pl.ds(0, NZ // 2), pl.ds(NZ // 2, NZ // 2)

    loads["ck"].wait()
    loads["cv"].wait()
    dims = (((0,), (0,)), ((), ()))
    for cols, cot, outs in (
        (slice(0, RK), cs_k, slice(0, KC)),
        (slice(RK, RK + RV), cs_v, slice(KC, NC)),
    ):
        b = basis[:, cols]
        upper = b.astype(jnp.bfloat16)
        lower = (b - upper.astype(jnp.float32)).astype(jnp.bfloat16)
        p = lax.dot_general(upper, cot[...], dims, preferred_element_type=jnp.float32)
        p += lax.dot_general(lower, cot[...], dims, preferred_element_type=jnp.float32)
        for b in range(NY):
            for i in range(outs.start // 128, NZ):
                if outs.start <= 128 * (i % 3) < outs.stop:
                    at = ROWS * b + 8 * (i // 3)
                    lanes = 128 * (i % 3) - outs.start
                    piece = p[at : at + 8, lanes : lanes + 128]
                    part[b, slots[i]] = piece
                    rs1_send[b, slots[i]] = piece.astype(jnp.bfloat16)

    for tiles, group in ((beyond, RS_REP_FAR), (near, RS_REP)):
        for d in FAR_Y:
            peer = ypeer(d, second)
            send(rs1_send.at[peer[1], tiles], rs1_recv.at[core, d - 1, tiles], group + core, peer)

        @pl.when(mover)
        def _():
            send(rs1_send.at[y, tiles], rs1_recv.at[0, NY - 1, tiles], group, other)

    pltpu.make_async_copy(mm, mm, moments_sem).wait()
    my_rows = pl.ds(pl.multiple_of(ROWS * y, ROWS), ROWS)

    gather, gather_last = gather_rows(
        z, y, kg, vg, krr, vrr, send, arrived, in_sems, zpeer, ypeer, first, second, other
    )

    @pl.when(mover)
    def _():
        send(mm.at[:, my_rows], twin_mm, MOMENTS_TWIN, other)
        gather()

    def normed_of(proj, first_old, second_old):
        first_new = first_decay * first_old + (1.0 - first_decay) * proj
        second_new = second_decay * second_old + (1.0 - second_decay) * proj * proj
        return first_new, second_new, first_new / (jnp.sqrt(second_new) + epsilon)

    def exchanges():
        for tiles, group, order in (
            (beyond, RS_REP_FAR, (6, 5, 7, 4, 8, 9)), (near, RS_REP, (3, 2, 10, 1, 11, 0)),
        ):
            arrived(rs1_recv.at[0, :, tiles], group)
            arrived(rs1_recv.at[1, pl.ds(0, NY - 1), tiles], group + 1)
            for d in order:
                slot = (d + NEAR) % NZ
                for c in range(2):
                    total = part[y, slot] if c else rs1_recv[0, NY - 1, slot].astype(jnp.float32)
                    for i in range(NY - 1):
                        total += rs1_recv[c, i, slot].astype(jnp.float32)
                    rs2_send[slot, c] = total
            for d in order:
                if d:
                    send(rs2_send.at[(d + NEAR) % NZ], rs2_recv.at[d - 1], RS_FS, zpeer(d, t))

        arrived(twin_mm, MOMENTS_TWIN)
        tile = rs2_send[NEAR]
        arrived(rs2_recv, RS_FS)
        for d in range(1, NZ):
            tile += rs2_recv[d - 1]
        ag[y, NEAR] = tile
        for d in FAR_Z:
            slot = (NEAR - d) % NZ
            send(ag.at[y, NEAR], ag.at[y, slot], AG_FS if slot < NZ // 2 else AG_FS_FAR, zpeer(d, t))

        def ag_send(ref, hops, rsem=None):
            send(ref, ref, AG_REP, ypeer(NY + hops, t), rsem)

        def ag_own(p, tiles):
            for hops, which in ((2, 0), (-2, 1)):
                ag_send(ag.at[y, tiles], hops, a2r.at[which, p])
            for hops in (1, -1):
                ag_send(ag.at[y, tiles], hops)

        def hand_over(block):
            send(ag.at[block, :, 0], ag.at[block, :, 0], AG_TWIN, other)

        def ag_pass(p, tiles):
            for hops, which in ((1, 0), (-1, 1)):
                ref = ag.at[lax.rem(y + NY - 2 * hops, NY), tiles]
                arrived(ref, rsem=a2r.at[which, p])
                ag_send(ref, hops)
                if which == p:
                    ag_send(ref, 2 * hops)

        arrived(ag.at[y, pl.ds(0, NZ // 2 - 1)], AG_FS)
        ag_own(0, near)
        arrived(ag.at[y, beyond], AG_FS_FAR)

        squares = jnp.zeros((8, 128), jnp.float32)
        for i in range(NZ):
            g, r = i % 3, 8 * (i // 3)
            at = pl.ds(pl.multiple_of(ROWS * y + r, 8), 8)
            n = normed_of(ag[y, slots[i], 1], mm[g, at], mm[3 + g, at])[2]
            squares += n * n
            n = normed_of(ag[y, slots[i], 0], twin_mm[g, r : r + 8], twin_mm[3 + g, r : r + 8])[2]
            squares += n * n
        qy[y] = squares
        for d in FAR_Y:
            send(qy.at[y], qy.at[y], SQ_REP, ypeer(d, t))
        ag_own(1, beyond)
        hand_over(y)

        ag_pass(0, near)

        arrived(qy.at[pl.ds(0, NY - 1)], SQ_REP)
        squares = qy[0]
        for i in range(1, NY):
            squares += qy[i]
        qt[x] = squares
        for d in range(1, NX):
            send(qt.at[x], qt.at[x], SQ_TP, (z, y, lax.rem(t + 2 * d, NT)))

        ag_pass(1, beyond)
        for hops in (2, -2):
            hand_over(lax.rem(y + NY + hops, NY))

        arrived(qt.at[pl.ds(0, NX - 1)], SQ_TP)
        squares = qt[0]
        for i in range(1, NX):
            squares += qt[i]
        total_sq[...] = squares
        send(total_sq, total_sq, SQ_TWIN, other)

        arrived(ag.at[pl.ds(0, NY - 3)], AG_REP)
        for hops in (1, -1, 3, -3, 4):
            hand_over(lax.rem(y + NY + hops, NY))

        sent(rs2_recv, RS_FS)
        sent(ag.at[y, pl.ds(0, NZ // 2 - 1)], AG_FS)
        sent(ag.at[y, beyond], AG_FS_FAR)
        sent(ag.at[pl.ds(0, NY - 1)], AG_REP)
        sent(qy.at[pl.ds(0, NY - 1)], SQ_REP)
        sent(qt.at[pl.ds(0, NX - 1)], SQ_TP)

    pl.when(adder)(exchanges)

    @pl.when(mover)
    def _():
        sent(twin_mm, MOMENTS_TWIN)
        arrived(ag.at[:, :, 0], AG_TWIN)
        arrived(total_sq, SQ_TWIN)

    for g in range(3):
        proj = jnp.concatenate([ag[b, slots[3 * i + g], core] for b in range(NY) for i in range(4)], axis=0)
        first_new, second_new, n = normed_of(proj, mm[g], mm[3 + g])
        mm[g] = first_new
        mm[3 + g] = second_new
        upper = n.astype(jnp.bfloat16)
        lower = (n - upper.astype(jnp.float32)).astype(jnp.bfloat16)
        normed[:, 128 * g : 128 * g + 128] = upper
        normed[:, NC + 128 * g : NC + 128 * g + 128] = lower

    squares = total_sq[...]
    whole = jnp.sum(jnp.sum(squares, axis=0, keepdims=True), axis=1, keepdims=True)
    entries = float(RK * DK + RV * DV)
    shrink_out[...] = jnp.broadcast_to(jnp.sqrt(entries / (entries + whole)), (8, 128))

    @pl.when(adder)
    def _():
        arrived(vg.at[1, 0, pl.ds(0, NY - 1)], VALUE_HOME)
        arrived(kg.at[1, pl.ds(0, NZ - 1), 0], KEY_HOME)
        arrived(vg.at[1, pl.ds(0, NZ - 1)], VALUE_RING_HOME)
        arrived(kg.at[1, :, pl.ds(0, NY - 1)], KEY_RING_HOME)
        sent(vg.at[1, z, NEAR_Y], VALUE_TWIN)
        sent(kg.at[1, NEAR, y], KEY_TWIN)
        sent(ag.at[:, :, 0], AG_TWIN)
        sent(total_sq, SQ_TWIN)
        sent(rs1_recv.at[0, pl.ds(0, NY - 1), near], RS_REP + 1)
        sent(rs1_recv.at[0, pl.ds(0, NY - 1), beyond], RS_REP_FAR + 1)

    @pl.when(mover)
    def _():
        gather_last()
        sent(rs1_recv.at[0, :, near], RS_REP)
        sent(rs1_recv.at[0, :, beyond], RS_REP_FAR)
        sent(vg.at[0, 0, pl.ds(0, NY - 1)], VALUE_HOME)
        sent(kg.at[0, pl.ds(0, NZ - 1), 0], KEY_HOME)
        sent(vg.at[0, pl.ds(0, NZ - 2)], VALUE_RING_HOME)
        sent(kg.at[0, :, pl.ds(0, NY - 2)], KEY_RING_HOME)
        sent(kg.at[:, :, pl.ds(0, NY - 1)], KEY_RING)
        sent(vg.at[:, pl.ds(0, NZ - 1)], VALUE_RING)

    sent(vg.at[0, 0, pl.ds(0, NY // 2 - 1)], VALUE)
    sent(vg.at[0, 0, pl.ds(0, NY // 2)], VALUE_FAR)
    sent(kg.at[0, pl.ds(0, NZ - 1), 0], KEY)


def gather_rows(z, y, kg, vg, krr, vrr, send, arrived, in_sems, zpeer, ypeer, mine, twin, other):
    def ring(block, chunks, me, n, peer_of, group, home, rsem):
        steps = n // 2

        def owner_of(direction, hops):
            return lax.rem(me + (n - hops if direction == 0 else hops), n)

        def carries(direction, s, c):
            return s < steps or (c < chunks // 2) == (direction == 0)

        def put(direction, s, c):
            owner, hop = owner_of(direction, s - 1), 1 if direction == 0 else n - 1
            rs = rsem.at[direction, s - 1, c]
            if s < steps:
                ref = block(slice(None), owner, c)
                send(ref, ref, group, peer_of(hop, mine), rs)
            else:
                for h, tp, sem in ((0, mine, rs), (1, twin, in_sems.at[home])):
                    send(block(h, owner, c), block(h, owner, c), group, peer_of(hop, tp), sem)

        def take(direction, s, c):
            owner = owner_of(direction, s)
            rs = rsem.at[direction, s - 1, c]
            if s == steps:
                arrived(block(0, owner, c), rsem=rs)
                return
            arrived(block(slice(None), owner, c), rsem=rs)
            if carries(direction, s + 1, c):
                put(direction, s + 1, c)
            send(block(1, owner, c), block(1, owner, c), home, other)

        def round_(s, chosen=range(chunks)):
            for c in chosen:
                for direction in range(2):
                    if s == 0:
                        put(direction, 1, c)
                    elif carries(direction, s, c):
                        take(direction, s, c)

        return round_

    kround = ring(
        lambda h, o, c: kg.at[h, pl.ds(c * (NZ // KCH), NZ // KCH), o],
        KCH, y, NY, ypeer, KEY_RING, KEY_RING_HOME, krr,
    )
    vround = ring(
        lambda h, o, c: vg.at[h, o, pl.ds(c * (NY // VCH), NY // VCH)],
        VCH, z, NZ, zpeer, VALUE_RING, VALUE_RING_HOME, vrr,
    )
    lower, upper = range(VCH // 2), range(VCH // 2, VCH)

    def home(ref, group):
        send(ref, ref, group, other)

    def gather():
        arrived(vg.at[1, z, NEAR_Y], VALUE_TWIN)
        arrived(vg.at[:, z, pl.ds(0, NY // 2 - 1)], VALUE)
        vround(0, lower)
        arrived(vg.at[:, z, pl.ds(NY // 2, NY // 2)], VALUE_FAR)
        vround(0, upper)
        for at, count in ((0, NEAR_Y), (NEAR_Y + 1, NY - NEAR_Y - 1)):
            home(vg.at[1, z, pl.ds(at, count)], VALUE_HOME)
        vround(1, lower)
        arrived(kg.at[1, NEAR, y], KEY_TWIN)
        arrived(kg.at[:, pl.ds(0, NZ - 1), y], KEY)
        kround(0)
        for at, count in ((0, NEAR), (NEAR + 1, NZ - NEAR - 1)):
            home(kg.at[1, pl.ds(at, count), y], KEY_HOME)
        vround(1, upper)
        vround(2, lower)
        kround(1)
        vround(2, upper)
        vround(3, lower)
        kround(2)
        vround(3, upper)
        vround(4, lower)
        vround(4, upper)
        vround(5, lower)
        vround(5, upper)
        kround(3)

    def gather_last():
        vround(6)
        kround(4)

    return gather, gather_last


def finish(
    kg, vg, fk, fv, wk, wv, mm, normed, shrink_in,
    wkn_hbm, wvn_hbm, m1kn_hbm, m2kn_hbm, m1vn_hbm, m2vn_hbm, sk_hbm, sv_hbm, kcopy_hbm, vcopy_hbm,
    kout, vout, ok, ov, osk, osv, out_sem,
):
    z, y, core = lax.axis_index("fs"), lax.axis_index("rep"), lax.rem(lax.axis_index("tp"), 2)
    outs = []

    def store(src, dst):
        copy = pltpu.make_async_copy(src, dst, out_sem.at[len(outs)])
        copy.start()
        outs.append(copy)

    for src, dst in (
        (0, m1kn_hbm), (1, m1vn_hbm.at[:, pl.ds(0, 128)]), (2, m1vn_hbm.at[:, pl.ds(128, 128)]),
        (3, m2kn_hbm), (4, m2vn_hbm.at[:, pl.ds(0, 128)]), (5, m2vn_hbm.at[:, pl.ds(128, 128)]),
    ):
        store(mm.at[src], dst)

    shrink = shrink_in[0:1, 0:1]

    def steps_of(rows, parts):
        key_step = value_step = 0.0
        for at in parts:
            key_step += jnp.dot(fk[rows, :], normed[:, at : at + KC], preferred_element_type=jnp.float32)
            value_step += jnp.dot(fv[rows, :], normed[:, at + KC : at + NC], preferred_element_type=jnp.float32)
        return shrink * key_step, shrink * value_step

    blocks = STEP // 256
    for b in range(D // STEP):
        rows = slice(b * STEP, b * STEP + STEP)
        key_step, value_step = steps_of(rows, (0,))
        kw = jnp.concatenate(
            [
                kg[core, lax.rem(blocks * b + i - z + NZ + NEAR, NZ)].reshape(256, KC)
                for i in range(blocks)
            ],
            axis=0,
        ).astype(jnp.float32)
        kout[rows, :] = (kw - learn_rate * key_step).astype(jnp.bfloat16)
        vw = jnp.concatenate(
            [vg[core, blocks * b + i, lax.rem(j - y + NY + NEAR_Y, NY)] for i in range(blocks) for j in range(NY)], axis=0
        ).astype(jnp.float32)
        vout[rows, :] = (vw - learn_rate * value_step).astype(jnp.bfloat16)
        store(kout.at[pl.ds(b * STEP, STEP)], kcopy_hbm.at[pl.ds(b * STEP, STEP)])
        store(vout.at[pl.ds(b * STEP, STEP)], vcopy_hbm.at[pl.ds(b * STEP, STEP)])

    key_step, value_step = steps_of(pl.ds(pl.multiple_of((z * NY + y) * ROWS, ROWS), ROWS), (0, NC))
    osk[...] = key_step
    osv[...] = value_step
    ok[...] = wk[...] - learn_rate * key_step
    ov[...] = wv[...] - learn_rate * value_step
    store(osk, sk_hbm)
    store(osv, sv_hbm)
    store(ok, wkn_hbm)
    store(ov, wvn_hbm)
    for copy in outs:
        copy.wait()


def body(*args):
    f32, bf16 = jnp.float32, jnp.bfloat16
    V, S = pltpu.VMEM, pltpu.SemaphoreType.DMA
    outs = [
        ((ROWS, KC), f32), ((ROWS, VC), f32), ((RK, KC), f32), ((RK, KC), f32), ((RV, VC), f32), ((RV, VC), f32),
        ((ROWS, KC), f32), ((ROWS, VC), f32), ((D, KC), bf16), ((D, VC), bf16),
    ]
    held = [
        V((2, NZ, NY, ROWS, KC), bf16), V((2, NZ, NY, ROWS, VC), bf16), V((D, RK), bf16), V((D, RV), bf16),
        V((ROWS, KC), f32), V((ROWS, VC), f32), V((6, RK, 128), f32), V((RK, 2 * NC), bf16), V((8, 128), f32),
    ]
    held_specs = [pl.BlockSpec(memory_space=V)] * len(held)
    middle = pl.pallas_call(
        kernel,
        name="projected_update",
        out_shape=held,
        in_specs=[pl.BlockSpec(memory_space=pltpu.HBM)] * 11,
        out_specs=held_specs,
        scratch_shapes=[
            V((TOK, D), bf16), V((TOK, KC), bf16), V((TOK, VC), bf16),
            V((TOK, RK + RV), f32), V((NY, NZ, 8, 128), f32), V((NY, NZ, 8, 128), bf16), V((2, NY, NZ, 8, 128), bf16),
            V((NZ, 2, 8, 128), f32), V((NZ - 1, 2, 8, 128), f32), V((NY, NZ, 2, 8, 128), f32),
            V((NX, 8, 128), f32), V((NY, 8, 128), f32), V((8, 128), f32), V((6, ROWS, 128), f32),
            S((2 + 3 * KCHUNKS + 2 + 1,)), S((GROUPS,)), S((GROUPS,)), S((2, 2)),
            S((2, NY // 2, KCH)), S((2, NZ // 2, VCH)),
        ],
        compiler_params=pltpu.CompilerParams(collective_id=0, has_side_effects=True, vmem_limit_bytes=VMEM_MAIN),
    )(*args)
    return pl.pallas_call(
        finish,
        name="finish",
        out_shape=[jax.ShapeDtypeStruct(s, dt) for s, dt in outs],
        in_specs=held_specs,
        out_specs=[pl.BlockSpec(memory_space=pltpu.HBM)] * len(outs),
        scratch_shapes=[
            V((D, KC), bf16), V((D, VC), bf16),
            V((ROWS, KC), f32), V((ROWS, VC), f32), V((ROWS, KC), f32), V((ROWS, VC), f32),
            S((10 + 2 * (D // STEP),)),
        ],
        compiler_params=pltpu.CompilerParams(vmem_limit_bytes=16 << 20),
    )(*middle)


def solution(mesh):
    tokens, rows, cols = P(("fs", "rep"), None), P(("fs", "rep"), "tp"), P(None, "tp")
    in_specs = (tokens, rows, rows, P(), P(), rows, rows, cols, cols, cols, cols)
    out_specs = (rows, rows, cols, cols, cols, cols, rows, rows, cols, cols)
    return jax.shard_map(body, mesh=mesh, in_specs=in_specs, out_specs=out_specs, check_vma=False)
```
